32 devices in a mesh: fs: 8 (over z, y), tp: 4 (over x, core).
Axes of the slice: x: 2, y: 2, z: 4, core: 2. Of those that a mesh axis runs over, the one named last changes fastest.
Arguments:
- h_saved: bfloat16 [4096, 4096], P('fs'), may hold values from -8 to 8
- y_saved: bfloat16 [4096, 2048], P('fs'), may hold values from -8 to 8
- d_gate: bfloat16 [4096, 2048], P('fs', 'tp'), may hold values from -0.25 to 0.25
- d_out: bfloat16 [4096, 4096], P('fs', 'tp'), may hold values from -0.25 to 0.25
- p_gate: bfloat16 [4096, 256], P('fs'), may hold values from -2 to 2
- p_out: bfloat16 [2048, 256], P('fs'), may hold values from -2 to 2
- w_gate: float32 [4096, 2048], P('fs', 'tp'), may hold values from -6 to 6
- w_out: float32 [2048, 4096], P('fs', 'tp'), may hold values from -6 to 6
- m_gate: float32 [256, 2048], P('fs', 'tp'), may hold values from -4 to 4
- m_out: float32 [256, 4096], P('fs', 'tp'), may hold values from -4 to 4
- v_gate: float32 [256, 2048], P('fs', 'tp'), may hold values from 0.02 to 0.2
- v_out: float32 [256, 4096], P('fs', 'tp'), may hold values from 0.02 to 0.2
Outputs:
- step_gate: float32 [4096, 2048], P('fs', 'tp')
- step_out: float32 [2048, 4096], P('fs', 'tp')
- moment_gate: float32 [256, 2048], P('fs', 'tp')
- moment_out: float32 [256, 4096], P('fs', 'tp')
- second_gate: float32 [256, 2048], P('fs', 'tp')
- second_out: float32 [256, 4096], P('fs', 'tp')
- copy_gate: bfloat16 [4096, 2048], P(None, 'tp')
- copy_out: bfloat16 [2048, 4096], P(None, 'tp')
The draws below stay inside these ranges and needn't reach their ends.
All inputs are finite; a program needn't handle non-finite values.
Results may differ from the reference program's by a relative error of at most 0.001.
Values may be sent and summed in bfloat16 or wider, within the bound.
A program may use at most 64 MiB of HBM per device.

```python
import math
import jax
import jax.numpy as jnp
from jax import lax

D = 4096
C = 2048
RANK = 256
TOKENS = 4096


def rising_draw(key, row_count, col_count, along_rows):
    noise = jnp.clip(jax.random.normal(key, (row_count, col_count), jnp.float32), -4.0, 4.0)
    spread = 4.0
    if along_rows:
        position = jnp.arange(row_count, dtype=jnp.float32) / max(row_count - 1, 1)
        return noise * (spread ** position)[:, None]
    position = jnp.arange(col_count, dtype=jnp.float32) / max(col_count - 1, 1)
    return noise * (spread ** position)[None, :]


def draw_p_gate(key, part):
    return (rising_draw(jax.random.fold_in(key, 11), D, RANK, True) * (0.5 / D ** 0.5)).astype(jnp.bfloat16)


def draw_p_out(key, part):
    return (rising_draw(jax.random.fold_in(key, 12), C, RANK, True) * (0.5 / C ** 0.5)).astype(jnp.bfloat16)


def draw_m_gate(key, part):
    return 0.2 * rising_draw(jax.random.fold_in(key, 13), RANK, C, False)


def draw_m_out(key, part):
    return 0.2 * rising_draw(jax.random.fold_in(key, 14), RANK, D, False)


def raised(array, rng, source, target, shards_of, factor):
    def block_of(dim):
        return (jnp.arange(array.shape[dim]) // (array.shape[dim] // shards_of)).reshape((-1,) + (1,) * (array.ndim - 1 - dim))

    one_side = jax.random.permutation(rng, shards_of)[block_of(target)]
    other_side = (block_of(target) + shards_of // 2) % shards_of
    return jnp.where((block_of(source) == one_side) | (block_of(source) == other_side), factor * array, array)


def block_scale(stream_key, shape, cuts, least, high):
    level = 1.0
    for dim, blocks in cuts:
        heights = jax.random.uniform(jax.random.fold_in(jax.random.fold_in(stream_key, 6), dim), (blocks,), jnp.float32, least / len(cuts), high / len(cuts))
        level = level * jnp.repeat(jnp.exp(heights), shape[dim] // blocks).reshape((-1,) + (1,) * (len(shape) - 1 - dim))
    return level


def gaussian(key, shape, deviation, limit, shards=(), kind=jnp.bfloat16):
    result = deviation * jax.random.normal(key, shape, jnp.float32)
    if shards:
        result = result * block_scale(key, shape, shards, -0.22, 0.18)
    return jnp.clip(result, -limit, limit).astype(kind)


def bell_draw_with(own_key, extent, scale, most, split, heavy, kind=jnp.bfloat16):
    array = scale * jax.random.normal(own_key, extent, jnp.float32)
    if split:
        array = array * block_scale(own_key, extent, split, -0.22, 0.18)
    return jnp.clip(raised(array, jax.random.fold_in(own_key, 3), *heavy), -most, most).astype(kind)


def setup_inputs(seed: int = 0) -> dict:
    key_of = jax.random.split(jax.random.key(seed), 13)
    return {
        "h_saved": bell_draw_with(key_of[0], (TOKENS, D), 1.0, 8.0, ((0, 8),), (0, 1, 8, 2.0)),
        "y_saved": bell_draw_with(key_of[1], (TOKENS, C), 1.0, 8.0, ((0, 8),), (0, 1, 8, 2.0)),
        "d_gate": gaussian(key_of[2], (TOKENS, C), (TOKENS ** -0.5), 0.25, ((0, 8), (1, 4))),
        "d_out": gaussian(key_of[3], (TOKENS, D), (TOKENS ** -0.5), 0.25, ((0, 8), (1, 4))),
        "p_gate": draw_p_gate(jax.random.fold_in(key_of[12], 71), 0),
        "p_out": draw_p_out(jax.random.fold_in(key_of[12], 71), 0),
        "w_gate": gaussian(key_of[6], (D, C), 1.0, 6.0, ((0, 8), (1, 4)), jnp.float32),
        "w_out": gaussian(key_of[7], (C, D), 1.0, 6.0, ((0, 8), (1, 4)), jnp.float32),
        "m_gate": draw_m_gate(jax.random.fold_in(key_of[12], 71), 0),
        "m_out": draw_m_out(jax.random.fold_in(key_of[12], 71), 0),
        "v_gate": jnp.clip(jnp.exp(math.log(0.2) - 2.3025851 * jax.random.uniform(key_of[10], (RANK, C), jnp.float32) ** block_scale(key_of[10], (RANK, C), ((0, 8), (1, 4)), -0.2, 0.2)), 0.02, 0.2),
        "v_out": jnp.clip(jnp.exp(math.log(0.2) - 2.3025851 * jax.random.uniform(key_of[11], (RANK, D), jnp.float32) ** block_scale(key_of[11], (RANK, D), ((0, 8), (1, 4)), -0.2, 0.2)), 0.02, 0.2),
    }


def one_matrix(saved, cotangent, factor, weight, first, second):
    grad = jnp.dot(saved.T, cotangent, preferred_element_type=jnp.float32)
    proj = jnp.dot(factor.astype(jnp.float32).T, grad, precision=lax.Precision.HIGHEST)
    moment = 0.9 * first + 0.1 * proj
    second_new = 0.95 * second + 0.05 * proj * proj
    normed = moment / jnp.sqrt(second_new)
    update = jnp.dot(factor.astype(jnp.float32), normed, precision=lax.Precision.HIGHEST)
    step = update * lax.rsqrt(jnp.mean(update * update) + 1e-06)
    copy_new = (weight - 0.1 * step).astype(jnp.bfloat16)
    return (step, moment, second_new, copy_new)

def reference(h_saved, y_saved, d_gate, d_out, p_gate, p_out, w_gate, w_out, m_gate, m_out, v_gate, v_out):
    step_gate, moment_gate, second_gate, copy_gate = one_matrix(h_saved, d_gate, p_gate, w_gate, m_gate, v_gate)
    step_out, moment_out, second_out, copy_out = one_matrix(y_saved, d_out, p_out, w_out, m_out, v_out)
    return (step_gate, step_out, moment_gate, moment_out, second_gate, second_out, copy_gate, copy_out)
```

```python
import functools
import jax
import jax.numpy as jnp
from jax import lax
from jax.experimental import pallas as pl
from jax.experimental.pallas import tpu as pltpu
from jax.sharding import PartitionSpec as P

BETA_ONE = 0.9
BETA_TWO = 0.95
LEARN_RATE = 0.1
EPSILON = 1e-06
MESH = pl.DeviceIdType.MESH
VMEM_SPEC = pl.BlockSpec(memory_space=pltpu.VMEM)
CORES = 2


def grid_of(count):
    inner = 1
    while 4 * inner * inner <= count:
        inner *= 2
    return count // inner, inner


def both(*conditions):
    kept = [c for c in conditions if c is not True]
    if not kept:
        return True
    return functools.reduce(jnp.logical_and, kept)


def when(condition, action):
    if condition is True:
        action()
    else:
        pl.when(condition)(action)


def greet(axis, spots):
    barrier = pltpu.get_barrier_semaphore()
    total = 0
    for valid, index in spots:

        def signal(index=index):
            pl.semaphore_signal(barrier, inc=1, device_id={axis: index}, device_id_type=MESH)

        when(valid, signal)
        total = total + (1 if valid is True else valid.astype(jnp.int32))
    pl.semaphore_wait(barrier, total)


def line_spots(me, grid):
    outer, inner = grid
    row, col = me // inner, me % inner
    spots = []
    if outer > 1:
        spots += [(row + 1 < outer, me + inner), (row > 0, me - inner)]
    if inner > 1:
        spots += [(col + 1 < inner, me + 1), (col > 0, me - 1)]
    return spots


def gather_kernel(axis, grid, pieces, count, *refs):
    ins, outs = refs[:count], refs[count : 2 * count]
    local_sem, send_sem, recv_sem = refs[2 * count :]
    outer, inner = grid
    me = lax.axis_index(axis)
    row, col = me // inner, me % inner
    locals_ = [pltpu.make_async_copy(ins[k], outs[k].at[me], local_sem.at[k]) for k in range(count)]
    for copy in locals_:
        copy.start()
    greet(axis, line_spots(me, grid))
    sends = []

    def copy_of(p, block, spot, target, own):
        k, start, rows, _ = pieces[p]
        here = outs[k].at[block, pl.ds(start, rows)]
        source = ins[k].at[pl.ds(start, rows)] if own else here
        return pltpu.make_async_remote_copy(
            src_ref=source,
            dst_ref=here,
            send_sem=send_sem.at[p, block, spot],
            recv_sem=recv_sem.at[p, block],
            device_id={axis: target},
            device_id_type=MESH,
        )

    def push(p, block, spot, target, valid, own=False):
        sends.append((p, block, spot, target, valid, own))
        when(valid, lambda: copy_of(p, block, spot, target, own).start())

    def land(p, block, valid):
        when(valid, lambda: copy_of(p, block, 0, me, False).wait_recv())

    events = []
    for p, (_, _, _, outer_first) in enumerate(pieces):
        if outer_first:
            first, second, pos1, pos2, step1, step2 = outer, inner, row, col, inner, 1
        else:
            first, second, pos1, pos2, step1, step2 = inner, outer, col, row, 1, inner
        spread = [(1, 0), (-1, 1)]

        def fits(pos, size, shift):
            return jnp.logical_and(pos + shift < size, pos + shift >= 0)

        def start_second(p, block, valid, own=False, pos2=pos2, second=second, step2=step2):
            if second > 1:
                for sign, spot in spread:
                    push(p, block, 2 + spot, me + sign * step2, both(valid, fits(pos2, second, sign)), own)

        def opening(p=p, pos1=pos1, first=first, step1=step1, start_second=start_second):
            if first > 1:
                for sign, spot in spread:
                    push(p, me, spot, me + sign * step1, fits(pos1, first, sign), True)
            start_second(p, me, True, True)

        events.append((0, p, opening))
        for s in range(1, first):
            for sign, spot in spread:

                def arrive(p=p, s=s, sign=sign, spot=spot, pos1=pos1, first=first, step1=step1, start_second=start_second):
                    block = me - sign * s * step1
                    valid = fits(pos1, first, -sign * s)
                    land(p, block, valid)
                    if s + 1 < first:
                        push(p, block, spot, me + sign * step1, both(valid, fits(pos1, first, sign)))
                    start_second(p, block, valid)

                events.append((s, p, arrive))
        for s in range(first):
            for sign1 in (1, -1) if s else (1,):
                for t in range(1, second):
                    for sign, spot in spread:

                        def relay(p=p, s=s, sign1=sign1, t=t, sign=sign, spot=spot, pos1=pos1, pos2=pos2, first=first, second=second, step1=step1, step2=step2):
                            block = me - sign1 * s * step1 - sign * t * step2
                            valid = fits(pos2, second, -sign * t)
                            if s:
                                valid = both(valid, fits(pos1, first, -sign1 * s))
                            land(p, block, valid)
                            if t + 1 < second:
                                push(p, block, 2 + spot, me + sign * step2, both(valid, fits(pos2, second, sign)))

                        events.append((s + t, p, relay))
    for _, _, event in sorted(events, key=lambda e: e[:2]):
        event()
    for p, block, spot, target, valid, own in sends:
        when(valid, lambda p=p, block=block, spot=spot, target=target, own=own: copy_of(p, block, spot, target, own).wait_send())
    for copy in locals_:
        copy.wait()


def gather(arrays, axis, size, grid, pieces, collective_id):
    count = len(arrays)
    return pl.pallas_call(
        functools.partial(gather_kernel, axis, grid, pieces, count),
        out_shape=[jax.ShapeDtypeStruct((size, *a.shape), a.dtype) for a in arrays],
        in_specs=[VMEM_SPEC] * count,
        out_specs=[VMEM_SPEC] * count,
        scratch_shapes=[
            pltpu.SemaphoreType.DMA((count,)),
            pltpu.SemaphoreType.DMA((len(pieces), size, 4)),
            pltpu.SemaphoreType.DMA((len(pieces), size)),
        ],
        compiler_params=pltpu.CompilerParams(
            collective_id=collective_id, has_side_effects=True, vmem_limit_bytes=60000000
        ),
    )(*arrays)


def scatter_kernel(axis, grid, orders, count, *refs):
    ins, outs = refs[:count], refs[count : 2 * count]
    rest = refs[2 * count :]
    stores, sems = rest[: 5 * count], rest[5 * count :]
    outer, inner = grid
    me = lax.axis_index(axis)
    row, col = me // inner, me % inner
    greet(axis, line_spots(me, grid))
    sends = []

    def line(k, phase, own, buffers, size, pos, step, sem_pair):
        send_sem, recv_sem = sem_pair

        def copy_of(way, dest, source):
            sign = 1 if way == 0 else -1
            return pltpu.make_async_remote_copy(
                src_ref=source,
                dst_ref=buffers[way].at[dest],
                send_sem=send_sem.at[way, dest],
                recv_sem=recv_sem.at[way, dest],
                device_id={axis: me + sign * step},
                device_id_type=MESH,
            )

        def round_(i):
            for way in (0, 1):
                dest = size - 1 - i if way == 0 else i
                valid = pos < dest if way == 0 else pos > dest
                edge = pos == 0 if way == 0 else pos == size - 1

                def from_edge(way=way, dest=dest):
                    copy_of(way, dest, own(dest)).start()

                def from_inside(way=way, dest=dest):
                    slot = buffers[way].at[dest]
                    copy_of(way, dest, slot).wait_recv()
                    slot[...] += own(dest)[...]
                    copy_of(way, dest, slot).start()

                when(both(valid, edge), from_edge)
                if size > 2:
                    when(both(valid, jnp.logical_not(edge)), from_inside)
                sends.append((valid, lambda way=way, dest=dest: copy_of(way, dest, buffers[way].at[dest]).wait_send()))

        def finish(total):
            total[...] = own(pos)[...]
            for way in (0, 1):

                def add(way=way):
                    slot = buffers[way].at[pos]
                    copy_of(way, pos, slot).wait_recv()
                    total[...] += slot[...]

                when(pos > 0 if way == 0 else pos < size - 1, add)

        return round_, finish

    jobs = []
    for k in range(count):
        up1, down1, middle, up2, down2 = stores[5 * k : 5 * k + 5]
        sem1, sem2 = sems[4 * k : 4 * k + 2], sems[4 * k + 2 : 4 * k + 4]
        ref = ins[k]
        if orders[k]:
            own1 = lambda d, ref=ref: ref.at[d]
            args1, args2 = (outer, row, inner), (inner, col, 1)
        else:
            own1 = lambda d, ref=ref: ref.at[:, d]
            args1, args2 = (inner, col, 1), (outer, row, inner)
        own2 = lambda d, middle=middle: middle.at[d]
        round1, finish1 = line(k, 0, own1, (up1, down1), *args1, sem1)
        round2, finish2 = line(k, 1, own2, (up2, down2), *args2, sem2)
        jobs.append((round1, finish1, round2, finish2, args1[0], args2[0], middle, outs[k]))
    span = max(j[4] for j in jobs) - 1 + max(j[5] for j in jobs)
    done = set()
    for tick in range(2 * (outer + inner)):
        for k, (round1, finish1, round2, finish2, size1, size2, middle, out) in enumerate(jobs):
            if tick < size1 - 1:
                round1(tick)
            elif tick == size1 - 1:
                finish1(middle)
                if size2 > 1:
                    round2(0)
            elif tick - size1 + 1 < size2 - 1:
                round2(tick - size1 + 1)
            elif k not in done:
                finish2(out)
                done.add(k)
    for valid, wait in sends:
        when(valid, wait)


def scatter(arrays, axis, grid, orders, collective_id):
    count = len(arrays)
    stores, sems = [], []
    for a, outer_first in zip(arrays, orders):
        outer, inner, rows, cols = a.shape
        first, second = (outer, inner) if outer_first else (inner, outer)
        stores += [pltpu.VMEM((first, second, rows, cols), a.dtype)] * 2
        stores += [pltpu.VMEM((second, rows, cols), a.dtype)] * 3
        sems += [pltpu.SemaphoreType.DMA((2, first))] * 2 + [pltpu.SemaphoreType.DMA((2, second))] * 2
    return pl.pallas_call(
        functools.partial(scatter_kernel, axis, grid, orders, count),
        out_shape=[jax.ShapeDtypeStruct(a.shape[2:], a.dtype) for a in arrays],
        in_specs=[VMEM_SPEC] * count,
        out_specs=[VMEM_SPEC] * count,
        scratch_shapes=stores + sems,
        compiler_params=pltpu.CompilerParams(
            collective_id=collective_id, has_side_effects=True, vmem_limit_bytes=60000000
        ),
    )(*arrays)


def total_kernel(sizes, x_ref, out_ref, near, far, mid, send_near, recv_near, send_far, recv_far):
    barrier = pltpu.get_barrier_semaphore()
    places = [("tp", sizes[1]), ("fs", sizes[0])]
    for axis, size in places:
        me = lax.axis_index(axis)
        for j in range(1, size):
            pl.semaphore_signal(barrier, inc=1, device_id={axis: (me + j) % size}, device_id_type=MESH)
    pl.semaphore_wait(barrier, sizes[0] + sizes[1] - 2)
    source = x_ref
    for (axis, size), held, send, recv, target in (
        (places[0], near, send_near, recv_near, mid),
        (places[1], far, send_far, recv_far, out_ref),
    ):
        me = lax.axis_index(axis)

        def copy_of(j, sign):
            return pltpu.make_async_remote_copy(
                src_ref=source,
                dst_ref=held.at[j],
                send_sem=send.at[j],
                recv_sem=recv.at[j],
                device_id={axis: (me + j) % size},
                device_id_type=MESH,
            )

        copies = [copy_of(j, 1) for j in range(1, size)]
        for copy in copies:
            copy.start()
        total = source[...]
        for j, copy in enumerate(copies, 1):
            copy.wait_recv()
            total = total + held[j]
        target[...] = total
        for copy in copies:
            copy.wait_send()
        source = mid


def total_over(x, sizes, collective_id):
    fs, tp = sizes
    return pl.pallas_call(
        functools.partial(total_kernel, sizes),
        out_shape=jax.ShapeDtypeStruct(x.shape, x.dtype),
        in_specs=[VMEM_SPEC],
        out_specs=VMEM_SPEC,
        scratch_shapes=[
            pltpu.VMEM((tp, *x.shape), x.dtype),
            pltpu.VMEM((fs, *x.shape), x.dtype),
            pltpu.VMEM(x.shape, x.dtype),
            pltpu.SemaphoreType.DMA((tp,)),
            pltpu.SemaphoreType.DMA((tp,)),
            pltpu.SemaphoreType.DMA((fs,)),
            pltpu.SemaphoreType.DMA((fs,)),
        ],
        compiler_params=pltpu.CompilerParams(collective_id=collective_id, has_side_effects=True),
    )(x)


def exact_dot(a, b):
    return jnp.dot(
        a.astype(jnp.float32), b.astype(jnp.float32), precision=lax.Precision.HIGHEST, preferred_element_type=jnp.float32
    )


def moments(first, second, proj):
    moment = BETA_ONE * first + (1.0 - BETA_ONE) * proj
    second_new = BETA_TWO * second + (1.0 - BETA_TWO) * proj * proj
    return moment, second_new, moment / jnp.sqrt(second_new)


def whole_rows(block):
    return (0, block.shape[0])


def on_device(
    fs, tp, h_saved, y_saved, d_gate, d_out, p_gate, p_out, w_gate, w_out, m_gate, m_out, v_gate, v_out
):
    fs_grid, tp_grid = grid_of(fs), (tp // CORES, CORES)
    rank = p_gate.shape[1]
    share = rank // tp
    mine = lax.axis_index("tp") * share
    slices = [lax.dynamic_slice_in_dim(p.T, mine, share, axis=0) for p in (p_gate, p_out)]
    wide = gather(slices, "fs", fs, fs_grid, ((0, 0, share, True), (1, 0, share, False)), 1)
    reduced = [
        lax.dot_general(
            jnp.transpose(g, (1, 0, 2)).reshape(share, -1),
            saved,
            (((1,), (1,)), ((), ())),
            preferred_element_type=jnp.float32,
        )
        for g, saved in zip(wide, (h_saved, y_saved))
    ]
    reduced = gather(reduced, "tp", tp, tp_grid, ((0, 0, share, True), (1, 0, share, True)), 2)
    parts = [
        exact_dot(r.reshape(rank, -1), d).reshape(*fs_grid, rank // fs, -1)
        for r, d in zip(reduced, (d_gate, d_out))
    ]
    proj_gate, proj_out = scatter(parts, "fs", fs_grid, (True, False), 3)
    moment_gate, second_gate, normed_gate = moments(m_gate, v_gate, proj_gate)
    moment_out, second_out, normed_out = moments(m_out, v_out, proj_out)
    rows = rank // fs
    whole = gather([normed_gate, normed_out], "fs", fs, fs_grid, ((0, 0, rows, False), (1, 0, rows, True)), 4)
    update_gate = exact_dot(p_gate, whole[0].reshape(rank, -1))
    update_out = exact_dot(p_out, whole[1].reshape(rank, -1))
    squares = jnp.concatenate(
        [jnp.full((8, 128), jnp.sum(u * u), jnp.float32) for u in (update_gate, update_out)], axis=0
    )
    squares = total_over(squares, (fs, tp), 5)
    step_gate = update_gate * lax.rsqrt(squares[0, 0] / (update_gate.size * fs * tp) + EPSILON)
    step_out = update_out * lax.rsqrt(squares[8, 0] / (update_out.size * fs * tp) + EPSILON)
    local_gate = (w_gate - LEARN_RATE * step_gate).astype(jnp.bfloat16)
    local_out = (w_out - LEARN_RATE * step_out).astype(jnp.bfloat16)
    half_gate, half_out = local_gate.shape[0] // 2, local_out.shape[0] // 2
    copies = gather(
        [local_gate, local_out],
        "fs",
        fs,
        fs_grid,
        ((0, 0, half_gate, False), (0, half_gate, half_gate, True), (1, 0, half_out, True), (1, half_out, half_out, True)),
        6,
    )
    copy_gate = copies[0].reshape(-1, local_gate.shape[1])
    copy_out = copies[1].reshape(-1, local_out.shape[1])
    return (step_gate, step_out, moment_gate, moment_out, second_gate, second_out, copy_gate, copy_out)


def solution(mesh):
    both_axes, rows = P("fs", "tp"), P("fs", None)
    fs, tp = mesh.shape["fs"], mesh.shape["tp"]
    return jax.shard_map(
        functools.partial(on_device, fs, tp),
        mesh=mesh,
        in_specs=(rows, rows, both_axes, both_axes, rows, rows) + (both_axes,) * 6,
        out_specs=(both_axes,) * 6 + (P(None, "tp"),) * 2,
        check_vma=False,
    )
```

```python
import functools
import jax
import jax.numpy as jnp
from jax import lax
from jax.experimental import pallas as pl
from jax.experimental.pallas import tpu as pltpu
from jax.sharding import PartitionSpec as P

BETA_ONE = 0.9
BETA_TWO = 0.95
LEARN_RATE = 0.1
EPSILON = 1e-06
MESH = pl.DeviceIdType.MESH
VMEM_SPEC = pl.BlockSpec(memory_space=pltpu.VMEM)
CORES = 2


def grid_of(count):
    inner = 1
    while 4 * inner * inner <= count:
        inner *= 2
    return count // inner, inner


def both(*conditions):
    kept = [c for c in conditions if c is not True]
    if not kept:
        return True
    return functools.reduce(jnp.logical_and, kept)


def when(condition, action):
    if condition is True:
        action()
    else:
        pl.when(condition)(action)


def greet(axis, spots):
    barrier = pltpu.get_barrier_semaphore()
    total = 0
    for valid, index in spots:

        def signal(index=index):
            pl.semaphore_signal(barrier, inc=1, device_id={axis: index}, device_id_type=MESH)

        when(valid, signal)
        total = total + (1 if valid is True else valid.astype(jnp.int32))
    pl.semaphore_wait(barrier, total)


def line_spots(me, grid):
    outer, inner = grid
    row, col = me // inner, me % inner
    spots = []
    if outer > 1:
        spots += [(row + 1 < outer, me + inner), (row > 0, me - inner)]
    if inner > 1:
        spots += [(col + 1 < inner, me + 1), (col > 0, me - 1)]
    return spots


def gather_kernel(axis, grid, pieces, count, *refs):
    ins, outs = refs[:count], refs[count : 2 * count]
    local_sem, send_sem, recv_sem = refs[2 * count :]
    me = lax.axis_index(axis)
    locals_ = [pltpu.make_async_copy(ins[k], outs[k].at[me], local_sem.at[k]) for k in range(count)]
    for copy in locals_:
        copy.start()
    greet(axis, line_spots(me, grid))
    gather_rounds(axis, grid, pieces, ins, outs, send_sem, recv_sem)
    for copy in locals_:
        copy.wait()


def gather_rounds(axis, grid, pieces, ins, outs, send_sem, recv_sem, beside=None):
    outer, inner = grid
    me = lax.axis_index(axis)
    row, col = me // inner, me % inner
    sends = []

    def copy_of(p, block, spot, target, own):
        k, start, rows, _ = pieces[p]
        here = outs[k].at[block, pl.ds(start, rows)]
        source = ins[k].at[pl.ds(start, rows)] if own and ins else here
        return pltpu.make_async_remote_copy(
            src_ref=source,
            dst_ref=here,
            send_sem=send_sem.at[p, block, spot],
            recv_sem=recv_sem.at[p, block],
            device_id={axis: target},
            device_id_type=MESH,
        )

    def push(p, block, spot, target, valid, own=False):
        sends.append((p, block, spot, target, valid, own))
        when(valid, lambda: copy_of(p, block, spot, target, own).start())

    def land(p, block, valid):
        when(valid, lambda: copy_of(p, block, 0, me, False).wait_recv())

    events = []
    for p, (_, _, _, outer_first) in enumerate(pieces):
        if outer_first:
            first, second, pos1, pos2, step1, step2 = outer, inner, row, col, inner, 1
        else:
            first, second, pos1, pos2, step1, step2 = inner, outer, col, row, 1, inner
        spread = [(1, 0), (-1, 1)]

        def fits(pos, size, shift):
            return jnp.logical_and(pos + shift < size, pos + shift >= 0)

        def start_second(p, block, valid, own=False, pos2=pos2, second=second, step2=step2):
            if second > 1:
                for sign, spot in spread:
                    push(p, block, 2 + spot, me + sign * step2, both(valid, fits(pos2, second, sign)), own)

        def opening(p=p, pos1=pos1, first=first, step1=step1, start_second=start_second):
            if first > 1:
                for sign, spot in spread:
                    push(p, me, spot, me + sign * step1, fits(pos1, first, sign), True)
            start_second(p, me, True, True)

        events.append((0, p, opening))
        for s in range(1, first):
            for sign, spot in spread:

                def arrive(p=p, s=s, sign=sign, spot=spot, pos1=pos1, first=first, step1=step1, start_second=start_second):
                    block = me - sign * s * step1
                    valid = fits(pos1, first, -sign * s)
                    land(p, block, valid)
                    if s + 1 < first:
                        push(p, block, spot, me + sign * step1, both(valid, fits(pos1, first, sign)))
                    start_second(p, block, valid)

                events.append((s, p, arrive))
        for s in range(first):
            for sign1 in (1, -1) if s else (1,):
                for t in range(1, second):
                    for sign, spot in spread:

                        def relay(p=p, s=s, sign1=sign1, t=t, sign=sign, spot=spot, pos1=pos1, pos2=pos2, first=first, second=second, step1=step1, step2=step2):
                            block = me - sign1 * s * step1 - sign * t * step2
                            valid = fits(pos2, second, -sign * t)
                            if s:
                                valid = both(valid, fits(pos1, first, -sign1 * s))
                            land(p, block, valid)
                            if t + 1 < second:
                                push(p, block, 2 + spot, me + sign * step2, both(valid, fits(pos2, second, sign)))

                        events.append((s + t, p, relay))
    if beside is not None:
        events.append((0, len(pieces), beside))
    for _, _, event in sorted(events, key=lambda e: e[:2]):
        event()
    for p, block, spot, target, valid, own in sends:
        when(valid, lambda p=p, block=block, spot=spot, target=target, own=own: copy_of(p, block, spot, target, own).wait_send())


def gather(arrays, axis, size, grid, pieces, collective_id):
    count = len(arrays)
    return pl.pallas_call(
        functools.partial(gather_kernel, axis, grid, pieces, count),
        out_shape=[jax.ShapeDtypeStruct((size, *a.shape), a.dtype) for a in arrays],
        in_specs=[VMEM_SPEC] * count,
        out_specs=[VMEM_SPEC] * count,
        scratch_shapes=[
            pltpu.SemaphoreType.DMA((count,)),
            pltpu.SemaphoreType.DMA((len(pieces), size, 4)),
            pltpu.SemaphoreType.DMA((len(pieces), size)),
        ],
        compiler_params=pltpu.CompilerParams(
            collective_id=collective_id, has_side_effects=True, vmem_limit_bytes=60000000
        ),
    )(*arrays)


def scatter_kernel(axis, grid, parts, pieces, *refs):
    ins, firsts, seconds = refs[:2], refs[2:4], refs[4:6]
    moment_outs, second_outs, wholes = refs[6:8], refs[8:10], refs[10:12]
    rest = refs[12:]
    count = len(parts)
    stores, sems = rest[: 6 * count], rest[6 * count : 10 * count]
    send_all, recv_all = rest[10 * count :]
    outer, inner = grid
    me = lax.axis_index(axis)
    row, col = me // inner, me % inner
    greet(axis, line_spots(me, grid))
    sends = []

    def line(k, phase, own, buffers, size, pos, step, sem_pair):
        send_sem, recv_sem = sem_pair

        def copy_of(way, dest, source):
            sign = 1 if way == 0 else -1
            return pltpu.make_async_remote_copy(
                src_ref=source,
                dst_ref=buffers[way].at[dest],
                send_sem=send_sem.at[way, dest],
                recv_sem=recv_sem.at[way, dest],
                device_id={axis: me + sign * step},
                device_id_type=MESH,
            )

        def round_(i):
            for way in (0, 1):
                dest = size - 1 - i if way == 0 else i
                valid = pos < dest if way == 0 else pos > dest
                edge = pos == 0 if way == 0 else pos == size - 1

                def from_edge(way=way, dest=dest):
                    copy_of(way, dest, own(dest)).start()

                def from_inside(way=way, dest=dest):
                    slot = buffers[way].at[dest]
                    copy_of(way, dest, slot).wait_recv()
                    slot[...] += own(dest)[...]
                    copy_of(way, dest, slot).start()

                when(both(valid, edge), from_edge)
                if size > 2:
                    when(both(valid, jnp.logical_not(edge)), from_inside)
                sends.append((valid, lambda way=way, dest=dest: copy_of(way, dest, buffers[way].at[dest]).wait_send()))

        def finish(total):
            total[...] = own(pos)[...]
            for way in (0, 1):

                def add(way=way):
                    slot = buffers[way].at[pos]
                    copy_of(way, pos, slot).wait_recv()
                    total[...] += slot[...]

                when(pos > 0 if way == 0 else pos < size - 1, add)

        return round_, finish

    jobs = []
    for k, (which, start, width, outer_first) in enumerate(parts):
        up1, down1, middle, up2, down2, proj = stores[6 * k : 6 * k + 6]
        sem1, sem2 = sems[4 * k : 4 * k + 2], sems[4 * k + 2 : 4 * k + 4]
        ref, cols = ins[which], pl.ds(start, width)
        if outer_first:
            own1 = lambda d, ref=ref, cols=cols: ref.at[d, :, :, cols]
            args1, args2 = (outer, row, inner), (inner, col, 1)
        else:
            own1 = lambda d, ref=ref, cols=cols: ref.at[:, d, :, cols]
            args1, args2 = (inner, col, 1), (outer, row, inner)
        own2 = lambda d, middle=middle: middle.at[d]
        round1, finish1 = line(k, 0, own1, (up1, down1), *args1, sem1)
        round2, finish2 = line(k, 1, own2, (up2, down2), *args2, sem2)

        def close(proj=proj, which=which, cols=cols, finish2=finish2):
            finish2(proj)
            moment, second, normed = moments(firsts[which][:, cols], seconds[which][:, cols], proj[...])
            moment_outs[which][:, cols] = moment
            second_outs[which][:, cols] = second
            wholes[which][me, :, cols] = normed

        jobs.append((round1, finish1, round2, close, args1[0], args2[0], middle))
    done = set()
    for tick in range(2 * (outer + inner)):
        for k, (round1, finish1, round2, close, size1, size2, middle) in enumerate(jobs):
            if tick < size1 - 1:
                round1(tick)
            elif tick == size1 - 1:
                finish1(middle)
                if size2 > 1:
                    round2(0)
            elif tick - size1 + 1 < size2 - 1:
                round2(tick - size1 + 1)
            elif k not in done:
                close()
                done.add(k)
    gather_rounds(axis, grid, pieces, None, wholes, send_all, recv_all)
    for valid, wait in sends:
        when(valid, wait)


def scatter(arrays, firsts, seconds, axis, grid, parts, pieces, collective_id):
    outer, inner = grid
    size = outer * inner
    stores, sems = [], []
    for which, _, width, outer_first in parts:
        rows = arrays[which].shape[2]
        first, second = (outer, inner) if outer_first else (inner, outer)
        stores += [pltpu.VMEM((first, second, rows, width), jnp.float32)] * 2
        stores += [pltpu.VMEM((second, rows, width), jnp.float32)] * 3
        stores += [pltpu.VMEM((rows, width), jnp.float32)]
        sems += [pltpu.SemaphoreType.DMA((2, first))] * 2 + [pltpu.SemaphoreType.DMA((2, second))] * 2
    small = [jax.ShapeDtypeStruct(m.shape, m.dtype) for m in firsts]
    wide = [jax.ShapeDtypeStruct((size, *m.shape), m.dtype) for m in firsts]
    return pl.pallas_call(
        functools.partial(scatter_kernel, axis, grid, parts, pieces),
        out_shape=small + small + wide,
        in_specs=[VMEM_SPEC] * 6,
        out_specs=[VMEM_SPEC] * 6,
        scratch_shapes=stores
        + sems
        + [
            pltpu.SemaphoreType.DMA((len(pieces), size, 4)),
            pltpu.SemaphoreType.DMA((len(pieces), size)),
        ],
        compiler_params=pltpu.CompilerParams(
            collective_id=collective_id, has_side_effects=True, vmem_limit_bytes=60000000
        ),
    )(*arrays, *firsts, *seconds)


def copies_kernel(sizes, grid, pieces, *refs):
    updates, weights, steps, copies_ = refs[:2], refs[2:4], refs[4:6], refs[6:8]
    x_ref, mid, out_ref, near, far = refs[8:13]
    send_near, recv_near, send_far, recv_far, send_all, recv_all = refs[13:]
    barrier = pltpu.get_barrier_semaphore()
    places = [("tp", sizes[1]), ("fs", sizes[0])]
    for axis, size in places:
        me = lax.axis_index(axis)
        for j in range(1, size):
            pl.semaphore_signal(barrier, inc=1, device_id={axis: (me + j) % size}, device_id_type=MESH)
    for k, update in enumerate(updates):
        rows, cols = update.shape
        value = update[...]
        lanes = jnp.sum((value * value).reshape(rows // 8, 8, cols), axis=0)
        x_ref[pl.ds(8 * k, 8), :] = sum(lanes[:, c : c + 128] for c in range(0, cols, 128))
    pl.semaphore_wait(barrier, sizes[0] + sizes[1] - 2)
    source = x_ref
    for (axis, size), held, send, recv, target in (
        (places[0], near, send_near, recv_near, mid),
        (places[1], far, send_far, recv_far, out_ref),
    ):
        me = lax.axis_index(axis)

        def copy_of(j, sign):
            return pltpu.make_async_remote_copy(
                src_ref=source,
                dst_ref=held.at[j],
                send_sem=send.at[j],
                recv_sem=recv.at[j],
                device_id={axis: (me + j) % size},
                device_id_type=MESH,
            )

        copies = [copy_of(j, 1) for j in range(1, size)]
        for copy in copies:
            copy.start()
        total = source[...]
        for j, copy in enumerate(copies, 1):
            copy.wait_recv()
            total = total + held[j]
        target[...] = total
        for copy in copies:
            copy.wait_send()
        source = mid


    me = lax.axis_index("fs")
    scales = []
    for k, update in enumerate(updates):
        total = jnp.sum(out_ref[pl.ds(8 * k, 8), :])
        scales.append(lax.rsqrt(total / (update.shape[0] * update.shape[1] * sizes[0] * sizes[1]) + EPSILON))
    for k, start, rows, _ in pieces:
        held = pl.ds(start, rows)
        step = updates[k][held, :] * scales[k]
        copies_[k][me, held, :] = (weights[k][held, :] - LEARN_RATE * step).astype(jnp.bfloat16)

    def write_steps():
        for k, update in enumerate(updates):
            steps[k][...] = update[...] * scales[k]

    gather_rounds("fs", grid, pieces, None, copies_, send_all, recv_all, write_steps)


def copies_of(updates, weights, sizes, grid, pieces, collective_id):
    fs, tp = sizes
    tile = (16, 128)
    return pl.pallas_call(
        functools.partial(copies_kernel, sizes, grid, pieces),
        out_shape=[jax.ShapeDtypeStruct(u.shape, u.dtype) for u in updates]
        + [jax.ShapeDtypeStruct((fs, *u.shape), jnp.bfloat16) for u in updates],
        in_specs=[VMEM_SPEC] * 4,
        out_specs=[VMEM_SPEC] * 4,
        scratch_shapes=[
            pltpu.VMEM(tile, jnp.float32),
            pltpu.VMEM(tile, jnp.float32),
            pltpu.VMEM(tile, jnp.float32),
            pltpu.VMEM((tp, *tile), jnp.float32),
            pltpu.VMEM((fs, *tile), jnp.float32),
            pltpu.SemaphoreType.DMA((tp,)),
            pltpu.SemaphoreType.DMA((tp,)),
            pltpu.SemaphoreType.DMA((fs,)),
            pltpu.SemaphoreType.DMA((fs,)),
            pltpu.SemaphoreType.DMA((len(pieces), fs, 4)),
            pltpu.SemaphoreType.DMA((len(pieces), fs)),
        ],
        compiler_params=pltpu.CompilerParams(
            collective_id=collective_id, has_side_effects=True, vmem_limit_bytes=60000000
        ),
    )(*updates, *weights)


def exact_dot(a, b):
    return jnp.dot(
        a.astype(jnp.float32), b.astype(jnp.float32), precision=lax.Precision.HIGHEST, preferred_element_type=jnp.float32
    )


def moments(first, second, proj):
    moment = BETA_ONE * first + (1.0 - BETA_ONE) * proj
    second_new = BETA_TWO * second + (1.0 - BETA_TWO) * proj * proj
    return moment, second_new, moment / jnp.sqrt(second_new)


def on_device(
    fs, tp, h_saved, y_saved, d_gate, d_out, p_gate, p_out, w_gate, w_out, m_gate, m_out, v_gate, v_out
):
    fs_grid, tp_grid = grid_of(fs), (tp // CORES, CORES)
    rank = p_gate.shape[1]
    share = rank // tp
    mine = lax.axis_index("tp") * share
    slices = [lax.dynamic_slice_in_dim(p.T, mine, share, axis=0) for p in (p_gate, p_out)]
    wide = gather(slices, "fs", fs, fs_grid, ((0, 0, share, True), (1, 0, share, False)), 1)
    reduced = [
        lax.dot_general(
            jnp.transpose(g, (1, 0, 2)).reshape(share, -1),
            saved,
            (((1,), (1,)), ((), ())),
            preferred_element_type=jnp.float32,
        )
        for g, saved in zip(wide, (h_saved, y_saved))
    ]
    reduced = gather(reduced, "tp", tp, tp_grid, ((0, 0, share, True), (1, 0, share, True)), 2)
    parts = [
        exact_dot(r.reshape(rank, -1), d).reshape(*fs_grid, rank // fs, -1)
        for r, d in zip(reduced, (d_gate, d_out))
    ]
    rows = rank // fs
    wide_gate, wide_out = m_gate.shape[1], m_out.shape[1] // 2
    moment_gate, moment_out, second_gate, second_out, whole_gate, whole_out = scatter(
        parts,
        (m_gate, m_out),
        (v_gate, v_out),
        "fs",
        fs_grid,
        ((0, 0, wide_gate, True), (1, 0, wide_out, False), (1, wide_out, wide_out, False)),
        ((0, 0, rows, False), (1, 0, rows, True)),
        3,
    )
    updates = [
        exact_dot(p, whole.reshape(rank, -1)) for p, whole in ((p_gate, whole_gate), (p_out, whole_out))
    ]
    half, quarter = w_gate.shape[0] // 2, w_out.shape[0] // 4
    step_gate, step_out, copy_gate, copy_out = copies_of(
        updates,
        (w_gate, w_out),
        (fs, tp),
        fs_grid,
        (
            (1, 0, quarter, False),
            (0, 0, half, True),
            (0, half, half, True),
            (1, quarter, quarter, True),
            (1, 2 * quarter, quarter, True),
            (1, 3 * quarter, quarter, True),
        ),
        5,
    )
    copy_gate = copy_gate.reshape(-1, w_gate.shape[1])
    copy_out = copy_out.reshape(-1, w_out.shape[1])
    return (step_gate, step_out, moment_gate, moment_out, second_gate, second_out, copy_gate, copy_out)


def solution(mesh):
    both_axes, rows = P("fs", "tp"), P("fs", None)
    fs, tp = mesh.shape["fs"], mesh.shape["tp"]
    return jax.shard_map(
        functools.partial(on_device, fs, tp),
        mesh=mesh,
        in_specs=(rows, rows, both_axes, both_axes, rows, rows) + (both_axes,) * 6,
        out_specs=(both_axes,) * 6 + (P(None, "tp"),) * 2,
        check_vma=False,
    )
```
